256 devices in a mesh: grp: 2 (over y), kv: 32 (over z, core), tp: 4 (over x).
Axes of the slice: x: 4, y: 2, z: 16, core: 2. Of those that a mesh axis runs over, the one named last changes fastest.
The devices are a block of a 4x16x16 slice.
Arguments:
- tokens: bfloat16 [16, 4096], P('grp', ('kv', 'tp')), parts along dimension 0, may hold values from -6 to 6
- input_gain: float32 [4096], P(('kv', 'tp')), may hold values from 0.1 to 1.9
- query_down: bfloat16 [4096, 1536], P(('kv', 'tp')), may hold values from -0.09375 to 0.09375
- latent_down: bfloat16 [4096, 1056], P(('kv', 'tp')), may hold values from -0.09375 to 0.09375
- query_gain: float32 [1536], replicated, may hold values from 0.1 to 1.9
- query_up: bfloat16 [1536, 3072], P('kv', 'tp'), may hold values from -0.15625 to 0.15625
- nope_gain: float32 [64], replicated, may hold values from 0.1 to 1.9
- query_rope_gain: float32 [32], replicated, may hold values from 0.1 to 1.9
- key_up: bfloat16 [1024, 2048], P('kv', 'tp'), may hold values from -0.1875 to 0.1875
- latent_gain: float32 [1024], replicated, may hold values from 0.1 to 1.9
- key_rope_gain: float32 [32], replicated, may hold values from 0.1 to 1.9
- latent_cache: bfloat16 [16, 12288, 1024], P('grp', 'kv'), parts along dimension 0, may hold values from -270 to 270
- rope_cache: bfloat16 [16, 32, 12288], P('grp', None, 'kv'), parts along dimension 0, may hold values from -4 to 4
- lengths: int32 [16], P('grp'), parts along dimension 0, may hold values from 3072 to 12288, as said below
- value_up: bfloat16 [1024, 2048], P('kv', 'tp'), may hold values from -6 to 6
- output_proj: bfloat16 [2048, 4096], P('tp', 'kv'), may hold values from -0.125 to 0.125
Outputs:
- attended: bfloat16 [16, 4096], P('grp', ('kv', 'tp')), parts along dimension 0
- new_latent: bfloat16 [16, 1024], P('grp'), parts along dimension 0
- new_rope_key: bfloat16 [16, 32], P('grp'), parts along dimension 0
The draws below stay inside these ranges and needn't reach their ends.
There are 2 independent parts, one for each index of `grp`. The reference program is written for one: setup_inputs(seed, part) draws one part's arguments, and reference() takes and returns one part's arrays. A program takes and returns all parts, laid end to end along the dimension named above; an argument that names none is the same for every part. Nothing has to cross between parts.
Inputs may be any that keep to these rules, and one draw needn't show every extreme that they name: Positions below a sequence's length hold its cache; the new token stands at position lengths; one sequence has length 12288 and one a quarter of 12288.
All inputs are finite; a program needn't handle non-finite values.
Results may differ from the reference program's by a relative error of at most 0.03.
Values may be sent and summed in bfloat16 or wider, within the bound.
No kernel may reach another device: no remote copies, remote signals or barrier semaphores. Data moves between devices by JAX's collectives and lax.ppermute only.
A program may use at most 64 MiB of HBM per device.

```python
import jax
import jax.numpy as jnp
from jax import lax

D = 4096
HEADS = 32
Q_RANK = 1536
KV_RANK = 1024
NOPE = 64
ROPE = 32
VDIM = 64
BATCH = 8
CONTEXT = 12288
N_TP = 4


def draw_lengths(key, part):
    drawn = jax.random.randint(key, (BATCH,), CONTEXT // 4, CONTEXT + 1)
    order = jax.random.permutation(jax.random.fold_in(key, 1), BATCH)
    return jnp.where(order == 0, CONTEXT, jnp.where(order == 1, CONTEXT // 4, drawn)).astype(jnp.int32)


def draw_latent_cache(key, part):
    result = jnp.clip(jax.random.normal(key, (BATCH, CONTEXT, KV_RANK), jnp.float32), -4.0, 4.0)
    return result.astype(jnp.bfloat16)


def steps_of(rng, dims, cuts, low, largest):
    level = 1.0
    for position, shards_of in cuts:
        draws = jax.random.uniform(jax.random.fold_in(jax.random.fold_in(rng, 6), position), (shards_of,), jnp.float32, low / len(cuts), largest / len(cuts))
        level = level * jnp.repeat(jnp.exp(draws), dims[position] // shards_of).reshape((-1,) + (1,) * (len(dims) - 1 - position))
    return level


def centred(key, shape, deviation, bound, cuts=(), held_as=jnp.bfloat16):
    values = jax.random.normal(key, shape, jnp.float32) * deviation
    if len(cuts) > 0:
        values = steps_of(key, shape, cuts, -0.22, 0.18) * values
    return jnp.clip(values, min=-bound, max=bound).astype(held_as)


def setup_inputs(seed: int = 0, part: int = 0) -> dict:
    key_of = jax.random.split(jax.random.key(seed), 17)
    part_keys = jax.random.split(jax.random.fold_in(key_of[16], part), 17)
    tokens = centred(part_keys[0], (BATCH, D), 1.0, 6.0, ((1, 128),))
    input_gain = jnp.clip(1.0 + 0.18 * jax.random.normal(key_of[1], (D,), jnp.float32), 0.1, 1.9)
    query_down = centred(key_of[2], (D, Q_RANK), D ** -0.5, 0.09375, ((0, 128),))
    latent_down = centred(key_of[3], (D, KV_RANK + ROPE), D ** -0.5, 0.09375, ((0, 128),))
    query_gain = jnp.clip(1.0 + 0.18 * jax.random.normal(key_of[4], (Q_RANK,), jnp.float32), 0.1, 1.9)
    query_up = centred(key_of[5], (Q_RANK, HEADS * (NOPE + ROPE)), Q_RANK ** -0.5, 0.15625, ((0, 32), (1, 4)))
    nope_gain = jnp.clip(1.0 + 0.18 * jax.random.normal(key_of[6], (NOPE,), jnp.float32), 0.1, 1.9)
    query_rope_gain = jnp.clip(1.0 + 0.18 * jax.random.normal(key_of[7], (ROPE,), jnp.float32), 0.1, 1.9)
    key_up = centred(key_of[8], (KV_RANK, HEADS * NOPE), KV_RANK ** -0.5, 0.1875, ((0, 32), (1, 4)))
    latent_gain = jnp.clip(1.0 + 0.18 * jax.random.normal(key_of[9], (KV_RANK,), jnp.float32), 0.1, 1.9)
    key_rope_gain = jnp.clip(1.0 + 0.18 * jax.random.normal(key_of[10], (ROPE,), jnp.float32), 0.1, 1.9)
    latent_cache = draw_latent_cache(jax.random.fold_in(jax.random.fold_in(key_of[16], part), 71), part)
    rope_cache = centred(part_keys[12], (BATCH, ROPE, CONTEXT), 1.0, 4.0, ((2, 32),))
    lengths = draw_lengths(jax.random.fold_in(jax.random.fold_in(key_of[16], part), 71), part)
    value_up = centred(key_of[14], (KV_RANK, HEADS * VDIM), 1.0, 6.0, ((0, 32), (1, 4)))
    output_proj = centred(key_of[15], (HEADS * VDIM, D), (HEADS * VDIM) ** -0.5, 0.125, ((0, 4), (1, 32)))
    return dict(tokens=tokens, input_gain=input_gain, query_down=query_down, latent_down=latent_down, query_gain=query_gain, query_up=query_up, nope_gain=nope_gain, query_rope_gain=query_rope_gain, key_up=key_up, latent_gain=latent_gain, key_rope_gain=key_rope_gain, latent_cache=latent_cache, rope_cache=rope_cache, lengths=lengths, value_up=value_up, output_proj=output_proj)


epsilon = 1e-06
theta = 10000.0
lowest = -1e+30

def normalize(values, gain):
    return values * lax.rsqrt(lax.optimization_barrier(jnp.mean(values * values, axis=-1, keepdims=True)) + epsilon) * gain.astype(jnp.float32)

def rotate(values, positions):
    half_width = values.shape[-1] // 2
    frequency = theta ** (-jnp.arange(half_width, dtype=jnp.float32) / half_width)
    angles = positions.astype(jnp.float32).reshape(positions.shape + (1,) * (values.ndim - 1)) * frequency
    cosines = jnp.cos(angles)
    sines = jnp.sin(angles)
    upper = values[..., :half_width]
    lower = values[..., half_width:]
    return jnp.concatenate([upper * cosines - lower * sines, upper * sines + lower * cosines], axis=-1)

def reference(tokens, input_gain, query_down, latent_down, query_gain, query_up, nope_gain, query_rope_gain, key_up, latent_gain, key_rope_gain, latent_cache, rope_cache, lengths, value_up, output_proj):
    floats = tokens.astype(jnp.float32)
    inverse = lax.rsqrt(lax.optimization_barrier(jnp.mean(floats * floats, axis=1, keepdims=True)) + epsilon)
    scaled = (floats * input_gain).astype(jnp.bfloat16)
    query_low = jnp.dot(scaled, query_down, preferred_element_type=jnp.float32) * inverse
    latent_low = jnp.dot(scaled, latent_down, preferred_element_type=jnp.float32) * inverse
    query_lat = normalize(query_low, query_gain).astype(jnp.bfloat16)
    queries = jnp.dot(query_lat, query_up, preferred_element_type=jnp.float32).reshape(BATCH, HEADS, NOPE + ROPE)
    query_nope = normalize(queries[..., :NOPE], nope_gain).astype(jnp.bfloat16)
    query_rope = rotate(normalize(queries[..., NOPE:], query_rope_gain), lengths).astype(jnp.bfloat16)
    key_heads = key_up.astype(jnp.float32).reshape(KV_RANK, HEADS, NOPE)
    query_latent = jnp.einsum('bhd,rhd->bhr', query_nope.astype(jnp.float32), key_heads).astype(jnp.bfloat16)
    new_latent = normalize(latent_low[:, :KV_RANK], latent_gain).astype(jnp.bfloat16)
    new_rope_key = rotate(normalize(latent_low[:, KV_RANK:], key_rope_gain), lengths).astype(jnp.bfloat16)
    score_scale = (NOPE + ROPE) ** (-0.5)

    def per_sequence(items):
        lat_query, rope_query, cache_rows, rope_rows, length, fresh_latent, fresh_rope = items
        cache_float = cache_rows.astype(jnp.float32)
        lat_float = lat_query.astype(jnp.float32)
        rope_float = rope_query.astype(jnp.float32)
        scores = (jnp.dot(lat_float, cache_float.T) + jnp.dot(rope_float, rope_rows.astype(jnp.float32))) * score_scale
        usable = jnp.arange(CONTEXT, dtype=jnp.int32) < length
        fresh = (jnp.dot(lat_float, fresh_latent.astype(jnp.float32)) + jnp.dot(rope_float, fresh_rope.astype(jnp.float32))) * score_scale
        masked = jnp.where(usable[None, :], scores, lowest)
        top = jnp.maximum(lax.optimization_barrier(jnp.max(masked, axis=1)), fresh)
        weights = jnp.where(usable[None, :], jnp.exp(masked - top[:, None]), 0.0)
        fresh_weight = jnp.exp(fresh - top)
        totals = lax.optimization_barrier(jnp.sum(weights, axis=1)) + fresh_weight
        rounded = lax.optimization_barrier(weights.astype(jnp.bfloat16)).astype(jnp.float32)
        rounded_fresh = lax.optimization_barrier(fresh_weight.astype(jnp.bfloat16)).astype(jnp.float32)
        summed = jnp.dot(rounded, cache_float) + rounded_fresh[:, None] * fresh_latent.astype(jnp.float32)[None, :]
        return (summed / totals[:, None]).astype(jnp.bfloat16)
    latent_out = lax.map(per_sequence, (query_latent, query_rope, latent_cache, rope_cache, lengths, new_latent, new_rope_key))
    value_heads = value_up.astype(jnp.float32).reshape(KV_RANK, HEADS, VDIM)
    head_out = jnp.einsum('bhr,rhe->bhe', latent_out.astype(jnp.float32), value_heads).reshape(BATCH, HEADS * VDIM).astype(jnp.bfloat16)
    block_rows = HEADS * VDIM // N_TP
    partials = jnp.einsum('bgk,gkd->bgd', head_out.astype(jnp.float32).reshape(BATCH, N_TP, block_rows), output_proj.astype(jnp.float32).reshape(N_TP, block_rows, D))
    partials = lax.optimization_barrier(partials.astype(jnp.bfloat16)).astype(jnp.float32)
    attended = lax.optimization_barrier(jnp.sum(partials, axis=1)).astype(jnp.bfloat16)
    return (attended, new_latent, new_rope_key)
```

```python
import jax
import jax.numpy as jnp
from jax import lax
from jax.experimental import pallas as pl
from jax.experimental.pallas import tpu as pltpu
from jax.sharding import Mesh
from jax.sharding import PartitionSpec as P

NOPE = 64
ROPE = 32
VDIM = 64
LANES = 128
KV = ("hi", "lo")
KV_TP = ("hi", "lo", "tp")

epsilon = 1e-06
theta = 10000.0
lowest = -1e30

f32 = jnp.float32
bf16 = jnp.bfloat16

IN_VMEM = pl.BlockSpec(memory_space=pltpu.VMEM)
IN_SMEM = pl.BlockSpec(memory_space=pltpu.SMEM)


def run(kernel, outs, *args, scratch=(), smem=()):
    return pl.pallas_call(
        kernel,
        out_shape=outs,
        in_specs=[IN_SMEM if i in smem else IN_VMEM for i in range(len(args))],
        out_specs=jax.tree.map(lambda _: IN_VMEM, outs),
        scratch_shapes=scratch,
    )(*args)


def exchange(x, axes):
    return lax.all_to_all(x, axes, 0, 0, tiled=True)


def from_others(x, axis):
    n = lax.axis_size(axis)
    return [lax.ppermute(x, axis, [(i, (i + s) % n) for i in range(n)]) for s in range(1, n)]


def lane_of(rows):
    return lax.broadcasted_iota(jnp.int32, (rows, LANES), 1)


def shifted(x, amount):
    return pltpu.roll(x, amount % LANES, 1) if amount % LANES else x


def window(x, start, length):
    tile, off = divmod(start, LANES)
    first = shifted(x[:, tile * LANES : (tile + 1) * LANES], -off)
    if off + length <= LANES:
        return first
    second = shifted(x[:, (tile + 1) * LANES : (tile + 2) * LANES], -off)
    return jnp.where(lane_of(x.shape[0]) < LANES - off, first, second)


def swapped_halves(x):
    half = ROPE // 2
    return jnp.where(lane_of(x.shape[0]) % ROPE < half, shifted(x, -half), shifted(x, half))


def split_two(x):
    top = x.astype(bf16).astype(f32)
    return top, (x - top).astype(bf16).astype(f32)


def dot(a, b):
    return jnp.dot(a, b, preferred_element_type=f32)


def compress(tokens, gain, query_down, latent_down, key_up, value_up, out, by_batch):
    kv, batch = out.shape[0], tokens.shape[0]
    heads = by_batch.shape[0]
    own = query_down.shape[1] // kv
    half = key_up.shape[0] // 2
    values = tokens[...].astype(f32)
    scaled = (values * gain[...]).astype(bf16)
    squares = jnp.sum(values * values, axis=1, keepdims=True)
    part_q = dot(scaled, query_down[...])
    part_l = dot(scaled, latent_down[...])
    lane = lane_of(batch)
    rest = jnp.concatenate([part_l[:, 8 * LANES :], jnp.zeros((batch, LANES - ROPE), f32)], axis=1)
    fixed = jnp.where(lane < 2 * ROPE, squares, shifted(rest, 2 * ROPE))
    for k in range(kv):
        out[k, 0:8, :] = jnp.where(lane < own, window(part_q, own * k, own), fixed).astype(bf16)
    for j in range(8):
        by_batch[:, j, :] = part_l[:, j * LANES : (j + 1) * LANES]
    for n in range(heads):
        tile = by_batch[n].astype(bf16)
        for k in range(n, kv, heads):
            out[k, 8:16, :] = tile
    low_lane = lane_of(half) < NOPE
    for row, weights in ((16, key_up), (16 + half, value_up)):
        for j in range(heads // 2):
            upper = weights[0:half, j * LANES : (j + 1) * LANES].astype(f32)
            lower = weights[half:, j * LANES : (j + 1) * LANES].astype(f32)
            pair = (
                jnp.where(low_lane, upper, shifted(lower, NOPE)).astype(bf16),
                jnp.where(low_lane, shifted(upper, NOPE), lower).astype(bf16),
            )
            for n in (0, 1):
                for k in range(2 * j + n, kv, heads):
                    out[k, row : row + half, :] = pair[n]


def gathered_sum(first, out):
    total = first[0, 0:16, :].astype(f32)
    for k in range(1, first.shape[0]):
        total = total + first[k, 0:16, :].astype(f32)
    out[...] = total.astype(bf16)


def unpack(first, key_head, value_head):
    half = key_head.shape[0] // first.shape[0] // 2
    for k in range(first.shape[0]):
        for row, out in ((16, key_head), (16 + half, value_head)):
            tile = first[k, row : row + half, :]
            out[2 * half * k : 2 * half * k + half, :] = tile
            out[2 * half * k + half : 2 * half * (k + 1), :] = shifted(
                tile.astype(f32), NOPE
            ).astype(bf16)


def expand(own, r1, r2, r3, gains, query_up, key_gain, latent_gain, cosines, sines, out, rope_out, rope_tile, latent_out, *, width):
    kv, batch = out.shape[0], out.shape[1]
    rows = query_up.shape[0]
    low = (own[...].astype(f32) + r2[...].astype(f32)) + (
        r1[...].astype(f32) + r3[...].astype(f32)
    )
    lane = lane_of(batch)
    upper = low[0:8]
    inverse = lax.rsqrt(upper[:, rows : rows + 1] / width + epsilon)
    upper = upper * inverse
    query_low = jnp.where(lane < rows, upper, 0.0)
    squares = jnp.sum(query_low * query_low, axis=1, keepdims=True)
    own_gain = gains[pl.ds(lax.axis_index(KV), 1), :]
    part = dot((query_low * own_gain)[:, :rows].astype(bf16), query_up[...])
    size = NOPE + ROPE
    heads = part.shape[1] // size
    for n in range(heads):
        tile = jnp.where(
            lane < size, window(part, size * n, size), jnp.where(lane == size, squares, 0.0)
        ).astype(bf16)
        for k in range(n, kv, heads):
            out[k] = tile
    in_rope = (lane >= 2 * ROPE) & (lane < 3 * ROPE)
    rope = jnp.where(in_rope, upper, 0.0)
    rope = (
        rope
        * lax.rsqrt(jnp.sum(rope * rope, axis=1, keepdims=True) / ROPE + epsilon)
        * key_gain[...]
    )
    rope = shifted(rope * cosines[...] + swapped_halves(rope) * sines[...], -2 * ROPE)
    rope = jnp.where(lane < ROPE, rope, 0.0)
    rope_tile[...] = rope
    rope_out[...] = rope[:, :ROPE].astype(bf16)
    chosen = lax.broadcasted_iota(jnp.int32, inverse.shape, 0) == lax.axis_index("lo")
    latent = low[8:16] * jnp.sum(jnp.where(chosen, inverse, 0.0), axis=0, keepdims=True)
    mean = jnp.sum(jnp.sum(latent * latent, axis=1, keepdims=True), axis=0, keepdims=True) / (
        latent.shape[0] * latent.shape[1]
    )
    latent_out[...] = (latent * lax.rsqrt(mean + epsilon) * latent_gain[...]).astype(bf16)


def absorb(parts, key_head, gain, cosines, sines, latent, out, *, rank):
    total = parts[0].astype(f32)
    for k in range(1, parts.shape[0]):
        total = total + parts[k].astype(f32)
    lane = lane_of(total.shape[0])
    size = NOPE + ROPE
    queries = total * lax.rsqrt(total[:, size : size + 1] / rank + epsilon)
    squared = queries * queries
    nope = lane < NOPE
    in_rope = (lane >= NOPE) & (lane < size)
    mean_nope = jnp.sum(jnp.where(nope, squared, 0.0), axis=1, keepdims=True) / NOPE
    mean_rope = jnp.sum(jnp.where(in_rope, squared, 0.0), axis=1, keepdims=True) / ROPE
    queries = (
        queries
        * jnp.where(nope, lax.rsqrt(mean_nope + epsilon), lax.rsqrt(mean_rope + epsilon))
        * gain[...]
    )
    rope = queries * cosines[...] + swapped_halves(queries) * sines[...]
    rope = jnp.where(lane < ROPE, shifted(rope, -NOPE), 0.0).astype(bf16)
    own = lax.dot_general(
        jnp.where(nope, queries, 0.0).astype(bf16),
        key_head[...],
        (((1,), (1,)), ((), ())),
        preferred_element_type=f32,
    ).astype(bf16)
    columns = own.shape[1]
    for n in range(out.shape[0]):
        out[n, :, :columns] = own
        out[n, :, columns : columns + LANES] = rope
        out[n, :, columns + LANES :] = latent[...]


def attend(lengths, third, cache, ropes, new_rope, out, new_latent, by_batch):
    heads, batch = third.shape[0], third.shape[1]
    rank = cache.shape[2]
    context = cache.shape[1]
    rows = heads * batch
    kv_index = lax.axis_index(KV)
    queries = third[...].reshape(rows, third.shape[2])
    latent_q = queries[:, :rank]
    rope_q = queries[:, rank : rank + LANES]
    by_batch[...] = third[:, :, rank + LANES :].astype(f32)
    fresh_latent = jnp.concatenate([by_batch[:, j, :] for j in range(batch)], axis=1)
    new_latent[...] = fresh_latent.astype(bf16)
    tiled = jnp.concatenate([fresh_latent] * heads, axis=0)
    tiled_rope = jnp.concatenate([new_rope[...].astype(bf16).astype(f32)] * heads, axis=0)
    scale = (NOPE + ROPE) ** (-0.5)
    fresh = (
        jnp.sum(latent_q.astype(f32) * tiled, axis=1, keepdims=True)
        + jnp.sum(rope_q.astype(f32) * tiled_rope, axis=1, keepdims=True)
    ) * scale
    leader = kv_index == 0
    fresh = jnp.where(leader, fresh, lowest)
    of_row = lax.broadcasted_iota(jnp.int32, (rows, 1), 0) % batch
    scores = jnp.zeros((rows, context), f32)
    limit = jnp.zeros((rows, 1), jnp.int32)
    for b in range(batch):
        part = lax.dot_general(
            latent_q, cache[b], (((1,), (1,)), ((), ())), preferred_element_type=f32
        ) + dot(rope_q[:, :ROPE], ropes[b])
        scores = jnp.where(of_row == b, part, scores)
        limit = jnp.where(of_row == b, lengths[b], limit)
    positions = kv_index * context + lax.broadcasted_iota(jnp.int32, (rows, context), 1)
    usable = positions < limit
    masked = jnp.where(usable, scores * scale, lowest)
    top = jnp.maximum(jnp.max(masked, axis=1, keepdims=True), fresh)
    top_hi, top_lo = split_two(top)
    top = top_hi + top_lo
    weights = jnp.where(usable, jnp.exp(masked - top), 0.0)
    fresh_weight = jnp.where(leader, jnp.exp(fresh - top), 0.0)
    totals = jnp.sum(weights, axis=1, keepdims=True) + fresh_weight
    summed = fresh_weight.astype(bf16).astype(f32) * tiled
    for b in range(batch):
        own = jnp.where(of_row == b, weights, 0.0).astype(bf16)
        summed = summed + dot(own, cache[b])
    total_hi, total_lo = split_two(totals)
    lane = lane_of(rows)
    stats = jnp.where(
        lane == 0,
        top_hi,
        jnp.where(lane == 1, top_lo, jnp.where(lane == 2, total_hi, total_lo)),
    )
    out[:, :, :rank] = summed.astype(bf16).reshape(heads, batch, rank)
    out[:, :, rank:] = stats.astype(bf16).reshape(heads, batch, LANES)


def combine(fourth, value_head, out):
    sources, batch = fourth.shape[0], fourth.shape[1]
    rank = value_head.shape[0]
    stats = fourth[:, :, rank:].astype(f32)
    tops = stats[:, :, 0:1] + stats[:, :, 1:2]
    part_totals = stats[:, :, 2:3] + stats[:, :, 3:4]
    top_hi, top_lo = split_two(jnp.max(tops, axis=0))
    factors = jnp.exp(tops - (top_hi + top_lo)[None])
    totals = jnp.sum(part_totals * factors, axis=0)
    summed = factors[0] * fourth[0, :, :rank].astype(f32)
    for s in range(1, sources):
        summed = summed + factors[s] * fourth[s, :, :rank].astype(f32)
    latent_out = (summed / jnp.where(totals > 0.0, totals, 1.0)).astype(bf16)
    head = dot(latent_out, value_head[...])
    total_hi, total_lo = split_two(totals)
    lane = lane_of(batch)
    tile = jnp.where(
        lane < VDIM,
        head,
        jnp.where(
            lane == VDIM,
            top_hi,
            jnp.where(lane == VDIM + 1, top_lo, jnp.where(lane == VDIM + 2, total_hi, total_lo)),
        ),
    ).astype(bf16)
    for k in range(out.shape[0]):
        out[k] = tile


def project(fifth, output_proj, out):
    kv, batch = fifth.shape[0], fifth.shape[1]
    heads = output_proj.shape[0] // VDIM
    blocks = fifth[...].astype(f32).reshape(kv // heads, heads, batch, LANES)
    tops = blocks[..., VDIM : VDIM + 1] + blocks[..., VDIM + 1 : VDIM + 2]
    factors = jnp.exp(tops - jnp.max(tops, axis=0, keepdims=True)) * (
        blocks[..., VDIM + 2 : VDIM + 3] + blocks[..., VDIM + 3 : VDIM + 4]
    )
    heads_out = jnp.sum(blocks * factors, axis=0) / jnp.sum(factors, axis=0)
    low_lane = lane_of(batch) < VDIM
    tiles = [
        jnp.where(low_lane, heads_out[n], shifted(heads_out[n + 1], VDIM))
        for n in range(0, heads, 2)
    ]
    out[...] = dot(jnp.concatenate(tiles, axis=1).astype(bf16), output_proj[...]).astype(bf16)


def finish(own, r1, r2, r3, out):
    total = (own[...].astype(f32) + r2[...].astype(f32)) + (
        r1[...].astype(f32) + r3[...].astype(f32)
    )
    columns = out.shape[1]
    index = lax.axis_index("tp")
    result = total[:, :columns]
    for t in range(1, LANES // columns):
        result = jnp.where(index == t, shifted(total, -t * columns)[:, :columns], result)
    out[...] = result.astype(bf16)


def body(
    tokens,
    input_gain,
    query_down,
    latent_down,
    query_gain,
    query_up,
    nope_gain,
    query_rope_gain,
    key_up,
    latent_gain,
    key_rope_gain,
    latent_cache,
    rope_cache,
    lengths,
    value_up,
    output_proj,
):
    batch = tokens.shape[0]
    kv = lax.axis_size(KV)
    lo = lax.axis_size("lo")
    tp = lax.axis_size("tp")
    width = tokens.shape[1] * kv * tp
    heads = query_up.shape[1] // (NOPE + ROPE)
    own_rows = query_up.shape[0]
    q_rank = own_rows * kv
    kv_rank = latent_cache.shape[2]
    half = key_up.shape[0] // 2
    assert heads == lo == batch == 8 and kv_rank == 8 * LANES and tp == 4

    def shape(*dims, dtype=bf16):
        return jax.ShapeDtypeStruct(dims, dtype)

    lanes = jnp.arange(LANES)
    angles = lengths.astype(f32)[:, None] * theta ** (
        -(lanes % (ROPE // 2)).astype(f32) / (ROPE // 2)
    )
    cosines = jnp.cos(angles)
    sines = jnp.sin(angles) * jnp.where(lanes % ROPE < ROPE // 2, -1.0, 1.0)
    gains = jnp.pad(query_gain.reshape(kv, own_rows), ((0, 0), (0, LANES - own_rows)))
    head_gain = jnp.pad(jnp.concatenate([nope_gain, query_rope_gain]), (0, ROPE))[None]
    key_gain = jnp.pad(key_rope_gain, (2 * ROPE, ROPE))[None]

    first = exchange(
        run(
            compress,
            shape(kv, 16 + 2 * half, LANES),
            tokens,
            input_gain[None],
            query_down,
            latent_down,
            key_up,
            value_up,
            scratch=[pltpu.VMEM((batch, 8, LANES), f32)],
        ),
        KV,
    )
    low = run(gathered_sum, shape(16, LANES), first)
    others = from_others(low, "tp")
    key_head, value_head = run(unpack, (shape(kv_rank, LANES), shape(kv_rank, LANES)), first)

    second, new_rope_key, rope_tile, latent_row = run(
        lambda *refs: expand(*refs, width=width),
        (
            shape(kv, batch, LANES),
            shape(batch, ROPE),
            shape(batch, LANES, dtype=f32),
            shape(8, LANES),
        ),
        low,
        *others,
        gains,
        query_up,
        key_gain,
        latent_gain.reshape(8, LANES),
        cosines,
        sines,
    )
    second = exchange(second, KV)
    third = exchange(
        run(
            lambda *refs: absorb(*refs, rank=q_rank),
            shape(lo, batch, kv_rank + 2 * LANES),
            second,
            key_head,
            head_gain,
            cosines,
            sines,
            latent_row,
        ),
        "lo",
    )
    fourth, new_latent = run(
        attend,
        (shape(heads, batch, kv_rank + LANES), shape(batch, kv_rank)),
        lengths,
        third,
        latent_cache,
        rope_cache,
        rope_tile,
        scratch=[pltpu.VMEM((batch, 8, LANES), f32)],
        smem=(0,),
    )
    fourth = exchange(fourth, "lo")
    fifth = exchange(run(combine, shape(kv, batch, LANES), fourth, value_head), KV)
    partial = run(project, shape(batch, output_proj.shape[1]), fifth, output_proj)
    attended = run(
        finish, shape(batch, output_proj.shape[1] // tp), partial, *from_others(partial, "tp")
    )
    return (attended, new_latent, new_rope_key)


def solution(mesh):
    kv, lo = mesh.shape["kv"], 8
    split = Mesh(
        mesh.devices.reshape(mesh.shape["grp"], kv // lo, lo, mesh.shape["tp"]),
        ("grp", "hi", "lo", "tp"),
    )
    placed = (
        P("grp", KV_TP),
        P(KV_TP),
        P(KV_TP, None),
        P(KV_TP, None),
        P(),
        P(KV, "tp"),
        P(),
        P(),
        P(KV, "tp"),
        P(),
        P(),
        P("grp", KV, None),
        P("grp", None, KV),
        P("grp"),
        P(KV, "tp"),
        P("tp", KV),
    )
    return jax.shard_map(
        body,
        mesh=split,
        in_specs=placed,
        out_specs=(P("grp", KV_TP), P("grp", None), P("grp", None)),
        check_vma=False,
    )
```

```python
import jax
import jax.numpy as jnp
from jax import lax
from jax.experimental import pallas as pl
from jax.experimental.pallas import tpu as pltpu
from jax.sharding import Mesh
from jax.sharding import PartitionSpec as P

NOPE = 64
ROPE = 32
VDIM = 64
LANES = 128
KV = ("hi", "lo")
KV_TP = ("hi", "lo", "tp")

epsilon = 1e-06
theta = 10000.0
lowest = -1e30

f32 = jnp.float32
bf16 = jnp.bfloat16

FLOPS = 1 << 32
VMEM_LIMIT = 16 << 20
IN_VMEM = pl.BlockSpec(memory_space=pltpu.VMEM)
IN_SMEM = pl.BlockSpec(memory_space=pltpu.SMEM)


def run(kernel, outs, *args, scratch=(), smem=(), vmem=VMEM_LIMIT, flops=0):
    return pl.pallas_call(
        kernel,
        out_shape=outs,
        in_specs=[IN_SMEM if i in smem else IN_VMEM for i in range(len(args))],
        out_specs=jax.tree.map(lambda _: IN_VMEM, outs),
        scratch_shapes=scratch,
        compiler_params=pltpu.CompilerParams(vmem_limit_bytes=vmem),
        cost_estimate=pl.CostEstimate(flops=flops, transcendentals=0, bytes_accessed=0),
    )(*args)


def exchange(x, axes):
    return lax.all_to_all(x, axes, 0, 0, tiled=True)


def from_others(x, axis):
    n = lax.axis_size(axis)
    return [lax.ppermute(x, axis, [(i, (i + s) % n) for i in range(n)]) for s in range(1, n)]


def lane_of(rows):
    return lax.broadcasted_iota(jnp.int32, (rows, LANES), 1)


def shifted(x, amount):
    return pltpu.roll(x, amount % LANES, 1) if amount % LANES else x


def window(x, start, length):
    tile, off = divmod(start, LANES)
    first = shifted(x[:, tile * LANES : (tile + 1) * LANES], -off)
    if off + length <= LANES:
        return first
    second = shifted(x[:, (tile + 1) * LANES : (tile + 2) * LANES], -off)
    return jnp.where(lane_of(x.shape[0]) < LANES - off, first, second)


def swapped_halves(x):
    half = ROPE // 2
    return jnp.where(lane_of(x.shape[0]) % ROPE < half, shifted(x, -half), shifted(x, half))


def split_two(x):
    top = x.astype(bf16).astype(f32)
    return top, (x - top).astype(bf16).astype(f32)


def dot(a, b):
    return jnp.dot(a, b, preferred_element_type=f32)


def compress(tokens, gain, query_down, latent_down, key_up, value_up, out, by_batch):
    kv, batch = out.shape[0], tokens.shape[0]
    heads = by_batch.shape[0]
    own = query_down.shape[1] // kv
    half = key_up.shape[0] // 2
    values = tokens[...].astype(f32)
    scaled = (values * gain[...]).astype(bf16)
    squares = jnp.sum(values * values, axis=1, keepdims=True)
    part_q = dot(scaled, query_down[...])
    part_l = dot(scaled, latent_down[...])
    lane = lane_of(batch)
    rest = jnp.concatenate([part_l[:, 8 * LANES :], jnp.zeros((batch, LANES - ROPE), f32)], axis=1)
    fixed = jnp.where(lane < 2 * ROPE, squares, shifted(rest, 2 * ROPE))
    for k in range(kv):
        out[k, 0:8, :] = jnp.where(lane < own, window(part_q, own * k, own), fixed).astype(bf16)
    for j in range(8):
        by_batch[:, j, :] = part_l[:, j * LANES : (j + 1) * LANES]
    for n in range(heads):
        tile = by_batch[n].astype(bf16)
        for k in range(n, kv, heads):
            out[k, 8:16, :] = tile
    low_lane = lane_of(half) < NOPE
    for row, weights in ((16, key_up), (16 + half, value_up)):
        for j in range(heads // 2):
            upper = weights[0:half, j * LANES : (j + 1) * LANES].astype(f32)
            lower = weights[half:, j * LANES : (j + 1) * LANES].astype(f32)
            pair = (
                jnp.where(low_lane, upper, shifted(lower, NOPE)).astype(bf16),
                jnp.where(low_lane, shifted(upper, NOPE), lower).astype(bf16),
            )
            for n in (0, 1):
                for k in range(2 * j + n, kv, heads):
                    out[k, row : row + half, :] = pair[n]


def gathered_sum(first, *refs):
    out = refs[-1]
    total = first[0, 0:16, :].astype(f32)
    for k in range(1, first.shape[0]):
        total = total + first[k, 0:16, :].astype(f32)
    out[...] = total.astype(bf16)


def unpack(first, key_head, value_head):
    half = key_head.shape[0] // first.shape[0] // 2
    for k in range(first.shape[0]):
        for row, out in ((16, key_head), (16 + half, value_head)):
            tile = first[k, row : row + half, :]
            out[2 * half * k : 2 * half * k + half, :] = tile
            out[2 * half * k + half : 2 * half * (k + 1), :] = shifted(
                tile.astype(f32), NOPE
            ).astype(bf16)


def expand(own, r1, r2, r3, gains, query_up, key_gain, latent_gain, cosines, sines, out, rope_out, rope_tile, latent_out, *, width):
    kv, batch = out.shape[0], out.shape[1]
    rows = query_up.shape[0]
    low = (own[...].astype(f32) + r2[...].astype(f32)) + (
        r1[...].astype(f32) + r3[...].astype(f32)
    )
    lane = lane_of(batch)
    upper = low[0:8]
    inverse = lax.rsqrt(upper[:, rows : rows + 1] / width + epsilon)
    upper = upper * inverse
    query_low = jnp.where(lane < rows, upper, 0.0)
    squares = jnp.sum(query_low * query_low, axis=1, keepdims=True)
    own_gain = gains[pl.ds(lax.axis_index(KV), 1), :]
    part = dot((query_low * own_gain)[:, :rows].astype(bf16), query_up[...])
    size = NOPE + ROPE
    heads = part.shape[1] // size
    for n in range(heads):
        tile = jnp.where(
            lane < size, window(part, size * n, size), jnp.where(lane == size, squares, 0.0)
        ).astype(bf16)
        for k in range(n, kv, heads):
            out[k] = tile
    in_rope = (lane >= 2 * ROPE) & (lane < 3 * ROPE)
    rope = jnp.where(in_rope, upper, 0.0)
    rope = (
        rope
        * lax.rsqrt(jnp.sum(rope * rope, axis=1, keepdims=True) / ROPE + epsilon)
        * key_gain[...]
    )
    rope = shifted(rope * cosines[...] + swapped_halves(rope) * sines[...], -2 * ROPE)
    rope = jnp.where(lane < ROPE, rope, 0.0)
    rope_tile[...] = rope
    rope_out[...] = rope[:, :ROPE].astype(bf16)
    chosen = lax.broadcasted_iota(jnp.int32, inverse.shape, 0) == lax.axis_index("lo")
    latent = low[8:16] * jnp.sum(jnp.where(chosen, inverse, 0.0), axis=0, keepdims=True)
    mean = jnp.sum(jnp.sum(latent * latent, axis=1, keepdims=True), axis=0, keepdims=True) / (
        latent.shape[0] * latent.shape[1]
    )
    latent_out[...] = (latent * lax.rsqrt(mean + epsilon) * latent_gain[...]).astype(bf16)


def absorb(parts, key_head, gain, cosines, sines, latent, out, *, rank):
    total = parts[0].astype(f32)
    for k in range(1, parts.shape[0]):
        total = total + parts[k].astype(f32)
    lane = lane_of(total.shape[0])
    size = NOPE + ROPE
    queries = total * lax.rsqrt(total[:, size : size + 1] / rank + epsilon)
    squared = queries * queries
    nope = lane < NOPE
    in_rope = (lane >= NOPE) & (lane < size)
    mean_nope = jnp.sum(jnp.where(nope, squared, 0.0), axis=1, keepdims=True) / NOPE
    mean_rope = jnp.sum(jnp.where(in_rope, squared, 0.0), axis=1, keepdims=True) / ROPE
    queries = (
        queries
        * jnp.where(nope, lax.rsqrt(mean_nope + epsilon), lax.rsqrt(mean_rope + epsilon))
        * gain[...]
    )
    rope = queries * cosines[...] + swapped_halves(queries) * sines[...]
    rope = jnp.where(lane < ROPE, shifted(rope, -NOPE), 0.0).astype(bf16)
    own = lax.dot_general(
        jnp.where(nope, queries, 0.0).astype(bf16),
        key_head[...],
        (((1,), (1,)), ((), ())),
        preferred_element_type=f32,
    ).astype(bf16)
    columns = own.shape[1]
    for n in range(out.shape[0]):
        out[n, :, :columns] = own
        out[n, :, columns : columns + LANES] = rope
        out[n, :, columns + LANES :] = latent[...]


def attend(lengths, third, cache, ropes, new_rope, out, new_latent, by_batch):
    heads, batch = third.shape[0], third.shape[1]
    rank = cache.shape[2]
    context = cache.shape[1]
    rows = heads * batch
    kv_index = lax.axis_index(KV)
    queries = third[...].reshape(rows, third.shape[2])
    latent_q = queries[:, :rank]
    rope_q = queries[:, rank : rank + LANES]
    by_batch[...] = third[:, :, rank + LANES :].astype(f32)
    fresh_latent = jnp.concatenate([by_batch[:, j, :] for j in range(batch)], axis=1)
    new_latent[...] = fresh_latent.astype(bf16)
    tiled = jnp.concatenate([fresh_latent] * heads, axis=0)
    tiled_rope = jnp.concatenate([new_rope[...].astype(bf16).astype(f32)] * heads, axis=0)
    scale = (NOPE + ROPE) ** (-0.5)
    fresh = (
        jnp.sum(latent_q.astype(f32) * tiled, axis=1, keepdims=True)
        + jnp.sum(rope_q.astype(f32) * tiled_rope, axis=1, keepdims=True)
    ) * scale
    leader = kv_index == 0
    fresh = jnp.where(leader, fresh, lowest)
    of_row = lax.broadcasted_iota(jnp.int32, (rows, 1), 0) % batch
    scores = jnp.zeros((rows, context), f32)
    limit = jnp.zeros((rows, 1), jnp.int32)
    for b in range(batch):
        part = lax.dot_general(
            latent_q, cache[b], (((1,), (1,)), ((), ())), preferred_element_type=f32
        ) + dot(rope_q[:, :ROPE], ropes[b])
        scores = jnp.where(of_row == b, part, scores)
        limit = jnp.where(of_row == b, lengths[b], limit)
    positions = kv_index * context + lax.broadcasted_iota(jnp.int32, (rows, context), 1)
    usable = positions < limit
    masked = jnp.where(usable, scores * scale, lowest)
    top = jnp.maximum(jnp.max(masked, axis=1, keepdims=True), fresh)
    top_hi, top_lo = split_two(top)
    top = top_hi + top_lo
    weights = jnp.where(usable, jnp.exp(masked - top), 0.0)
    fresh_weight = jnp.where(leader, jnp.exp(fresh - top), 0.0)
    totals = jnp.sum(weights, axis=1, keepdims=True) + fresh_weight
    summed = fresh_weight.astype(bf16).astype(f32) * tiled
    for b in range(batch):
        own = jnp.where(of_row == b, weights, 0.0).astype(bf16)
        summed = summed + dot(own, cache[b])
    total_hi, total_lo = split_two(totals)
    lane = lane_of(rows)
    stats = jnp.where(
        lane == 0,
        top_hi,
        jnp.where(lane == 1, top_lo, jnp.where(lane == 2, total_hi, total_lo)),
    )
    out[:, :, :rank] = summed.astype(bf16).reshape(heads, batch, rank)
    out[:, :, rank:] = stats.astype(bf16).reshape(heads, batch, LANES)


def combine(fourth, value_head, out):
    sources, batch = fourth.shape[0], fourth.shape[1]
    rank = value_head.shape[0]
    stats = fourth[:, :, rank:].astype(f32)
    tops = stats[:, :, 0:1] + stats[:, :, 1:2]
    part_totals = stats[:, :, 2:3] + stats[:, :, 3:4]
    top_hi, top_lo = split_two(jnp.max(tops, axis=0))
    factors = jnp.exp(tops - (top_hi + top_lo)[None])
    totals = jnp.sum(part_totals * factors, axis=0)
    summed = factors[0] * fourth[0, :, :rank].astype(f32)
    for s in range(1, sources):
        summed = summed + factors[s] * fourth[s, :, :rank].astype(f32)
    latent_out = (summed / jnp.where(totals > 0.0, totals, 1.0)).astype(bf16)
    head = dot(latent_out, value_head[...])
    total_hi, total_lo = split_two(totals)
    lane = lane_of(batch)
    tile = jnp.where(
        lane < VDIM,
        head,
        jnp.where(
            lane == VDIM,
            top_hi,
            jnp.where(lane == VDIM + 1, top_lo, jnp.where(lane == VDIM + 2, total_hi, total_lo)),
        ),
    ).astype(bf16)
    for k in range(out.shape[0]):
        out[k] = tile


def project(fifth, output_proj, out):
    kv, batch = fifth.shape[0], fifth.shape[1]
    heads = output_proj.shape[0] // VDIM
    blocks = fifth[...].astype(f32).reshape(kv // heads, heads, batch, LANES)
    tops = blocks[..., VDIM : VDIM + 1] + blocks[..., VDIM + 1 : VDIM + 2]
    factors = jnp.exp(tops - jnp.max(tops, axis=0, keepdims=True)) * (
        blocks[..., VDIM + 2 : VDIM + 3] + blocks[..., VDIM + 3 : VDIM + 4]
    )
    heads_out = jnp.sum(blocks * factors, axis=0) / jnp.sum(factors, axis=0)
    low_lane = lane_of(batch) < VDIM
    tiles = [
        jnp.where(low_lane, heads_out[n], shifted(heads_out[n + 1], VDIM))
        for n in range(0, heads, 2)
    ]
    out[...] = dot(jnp.concatenate(tiles, axis=1).astype(bf16), output_proj[...]).astype(bf16)


def finish(own, r1, r2, r3, out):
    total = (own[...].astype(f32) + r2[...].astype(f32)) + (
        r1[...].astype(f32) + r3[...].astype(f32)
    )
    columns = out.shape[1]
    index = lax.axis_index("tp")
    result = total[:, :columns]
    for t in range(1, LANES // columns):
        result = jnp.where(index == t, shifted(total, -t * columns)[:, :columns], result)
    out[...] = result.astype(bf16)


def body(
    tokens,
    input_gain,
    query_down,
    latent_down,
    query_gain,
    query_up,
    nope_gain,
    query_rope_gain,
    key_up,
    latent_gain,
    key_rope_gain,
    latent_cache,
    rope_cache,
    lengths,
    value_up,
    output_proj,
):
    batch = tokens.shape[0]
    kv = lax.axis_size(KV)
    lo = lax.axis_size("lo")
    tp = lax.axis_size("tp")
    width = tokens.shape[1] * kv * tp
    heads = query_up.shape[1] // (NOPE + ROPE)
    own_rows = query_up.shape[0]
    q_rank = own_rows * kv
    kv_rank = latent_cache.shape[2]
    half = key_up.shape[0] // 2
    assert heads == lo == batch == 8 and kv_rank == 8 * LANES and tp == 4

    def shape(*dims, dtype=bf16):
        return jax.ShapeDtypeStruct(dims, dtype)

    lanes = jnp.arange(LANES)
    angles = lengths.astype(f32)[:, None] * theta ** (
        -(lanes % (ROPE // 2)).astype(f32) / (ROPE // 2)
    )
    cosines = jnp.cos(angles)
    sines = jnp.sin(angles) * jnp.where(lanes % ROPE < ROPE // 2, -1.0, 1.0)
    gains = jnp.pad(query_gain.reshape(kv, own_rows), ((0, 0), (0, LANES - own_rows)))
    head_gain = jnp.pad(jnp.concatenate([nope_gain, query_rope_gain]), (0, ROPE))[None]
    key_gain = jnp.pad(key_rope_gain, (2 * ROPE, ROPE))[None]

    first = exchange(
        run(
            compress,
            shape(kv, 16 + 2 * half, LANES),
            tokens,
            input_gain[None],
            query_down,
            latent_down,
            key_up,
            value_up,
            scratch=[pltpu.VMEM((batch, 8, LANES), f32)],
            vmem=60 << 20,
        ),
        KV,
    )
    low = run(gathered_sum, shape(16, LANES), first, cosines, sines, gains, head_gain, key_gain, flops=FLOPS)
    others = from_others(low, "tp")
    key_head, value_head = run(unpack, (shape(kv_rank, LANES), shape(kv_rank, LANES)), first, flops=FLOPS)

    second, new_rope_key, rope_tile, latent_row = run(
        lambda *refs: expand(*refs, width=width),
        (
            shape(kv, batch, LANES),
            shape(batch, ROPE),
            shape(batch, LANES, dtype=f32),
            shape(8, LANES),
        ),
        low,
        *others,
        gains,
        query_up,
        key_gain,
        latent_gain.reshape(8, LANES),
        cosines,
        sines,
        flops=FLOPS,
    )
    second = exchange(second, KV)
    third = exchange(
        run(
            lambda *refs: absorb(*refs, rank=q_rank),
            shape(lo, batch, kv_rank + 2 * LANES),
            second,
            key_head,
            head_gain,
            cosines,
            sines,
            latent_row,
            flops=FLOPS,
        ),
        "lo",
    )
    fourth, new_latent = run(
        attend,
        (shape(heads, batch, kv_rank + LANES), shape(batch, kv_rank)),
        lengths,
        third,
        latent_cache,
        rope_cache,
        rope_tile,
        scratch=[pltpu.VMEM((batch, 8, LANES), f32)],
        smem=(0,),
    )
    fourth = exchange(fourth, "lo")
    fifth = exchange(run(combine, shape(kv, batch, LANES), fourth, value_head), KV)
    partial = run(project, shape(batch, output_proj.shape[1]), fifth, output_proj)
    attended = run(
        finish, shape(batch, output_proj.shape[1] // tp), partial, *from_others(partial, "tp")
    )
    return (attended, new_latent, new_rope_key)


def solution(mesh):
    kv, lo = mesh.shape["kv"], 8
    split = Mesh(
        mesh.devices.reshape(mesh.shape["grp"], kv // lo, lo, mesh.shape["tp"]),
        ("grp", "hi", "lo", "tp"),
    )
    placed = (
        P("grp", KV_TP),
        P(KV_TP),
        P(KV_TP, None),
        P(KV_TP, None),
        P(),
        P(KV, "tp"),
        P(),
        P(),
        P(KV, "tp"),
        P(),
        P(),
        P("grp", KV, None),
        P("grp", None, KV),
        P("grp"),
        P(KV, "tp"),
        P("tp", KV),
    )
    return jax.shard_map(
        body,
        mesh=split,
        in_specs=placed,
        out_specs=(P("grp", KV_TP), P("grp", None), P("grp", None)),
        check_vma=False,
    )
```

```python
import jax
import jax.numpy as jnp
from jax import lax
from jax.experimental import pallas as pl
from jax.experimental.pallas import tpu as pltpu
from jax.sharding import Mesh
from jax.sharding import PartitionSpec as P

NOPE = 64
ROPE = 32
VDIM = 64
LANES = 128
CUT = 32
EDGE = 52
KV = ("hi", "lo")
KV_TP = ("hi", "lo", "tp")

epsilon = 1e-06
theta = 10000.0
lowest = -1e30

f32 = jnp.float32
bf16 = jnp.bfloat16

FLOPS = 1 << 32
VMEM_LIMIT = 16 << 20
IN_VMEM = pl.BlockSpec(memory_space=pltpu.VMEM)
IN_SMEM = pl.BlockSpec(memory_space=pltpu.SMEM)


def run(kernel, outs, *args, scratch=(), smem=(), vmem=VMEM_LIMIT, flops=0):
    return pl.pallas_call(
        kernel,
        out_shape=outs,
        in_specs=[IN_SMEM if i in smem else IN_VMEM for i in range(len(args))],
        out_specs=jax.tree.map(lambda _: IN_VMEM, outs),
        scratch_shapes=scratch,
        compiler_params=pltpu.CompilerParams(vmem_limit_bytes=vmem),
        cost_estimate=pl.CostEstimate(flops=flops, transcendentals=0, bytes_accessed=0),
    )(*args)


def exchange(x, axes):
    return lax.all_to_all(x, axes, 0, 0, tiled=True)


def lane_of(rows):
    return lax.broadcasted_iota(jnp.int32, (rows, LANES), 1)


def shifted(x, amount):
    return pltpu.roll(x, amount % LANES, 1) if amount % LANES else x


def window(x, start, length):
    tile, off = divmod(start, LANES)
    first = shifted(x[:, tile * LANES : (tile + 1) * LANES], -off)
    if off + length <= LANES:
        return first
    second = shifted(x[:, (tile + 1) * LANES : (tile + 2) * LANES], -off)
    return jnp.where(lane_of(x.shape[0]) < LANES - off, first, second)


def swapped_halves(x):
    half = ROPE // 2
    return jnp.where(lane_of(x.shape[0]) % ROPE < half, shifted(x, -half), shifted(x, half))


def split_two(x):
    top = x.astype(bf16).astype(f32)
    return top, (x - top).astype(bf16).astype(f32)


def dot(a, b):
    return jnp.dot(a, b, preferred_element_type=f32)


def compress(tokens, gain, query_down, latent_down, key_up, value_up, out, by_batch):
    kv, batch = out.shape[0], tokens.shape[0]
    heads = by_batch.shape[0]
    own = query_down.shape[1] // kv
    values = tokens[...].astype(f32)
    scaled = (values * gain[...]).astype(bf16)
    squares = jnp.sum(values * values, axis=1, keepdims=True)
    part_q = dot(scaled, query_down[...])
    part_l = dot(scaled, latent_down[...])
    lane = lane_of(batch)
    rest = jnp.concatenate([part_l[:, 8 * LANES :], jnp.zeros((batch, LANES - ROPE), f32)], axis=1)
    fixed = jnp.where(lane < 2 * ROPE, squares, shifted(rest, 2 * ROPE))
    for j in range(8):
        by_batch[:, j, :] = part_l[:, j * LANES : (j + 1) * LANES]
    for n in range(heads):
        latent = by_batch[n]
        shared = fixed
        for m in range(LANES // CUT):
            shared = jnp.where(
                lane == EDGE + m, shifted(latent, EDGE + m - (m * CUT + CUT - 1)), shared
            )
        for k in range(n, kv, heads):
            tile = jnp.where(lane < own, window(part_q, own * k, own), shared)
            tile = jnp.where(
                lane < LANES - CUT, tile, shifted(latent, LANES - CUT - k // heads * CUT)
            )
            out[k, 0:8, :] = tile.astype(bf16)
    half = key_up.shape[0] // 2
    low_lane = lane_of(half) < NOPE
    for row, weights in ((8, key_up), (8 + half, value_up)):
        for j in range(heads // 2):
            upper = weights[0:half, j * LANES : (j + 1) * LANES].astype(f32)
            lower = weights[half:, j * LANES : (j + 1) * LANES].astype(f32)
            pair = (
                jnp.where(low_lane, upper, shifted(lower, NOPE)).astype(bf16),
                jnp.where(low_lane, shifted(upper, NOPE), lower).astype(bf16),
            )
            for n in (0, 1):
                for k in range(2 * j + n, kv, heads):
                    out[k, row : row + half, :] = pair[n]


def gathered(first, *refs):
    low, key_head, value_head = refs[-3:]
    half = key_head.shape[0] // first.shape[0] // 2
    total = first[0, 0:8, :].astype(f32)
    for k in range(1, first.shape[0]):
        total = total + first[k, 0:8, :].astype(f32)
    for t in range(low.shape[0]):
        low[t] = total.astype(bf16)
    for k in range(first.shape[0]):
        for row, out in ((8, key_head), (8 + half, value_head)):
            tile = first[k, row : row + half, :]
            out[2 * half * k : 2 * half * k + half, :] = tile
            out[2 * half * k + half : 2 * half * (k + 1), :] = shifted(
                tile.astype(f32), NOPE
            ).astype(bf16)


def total_of(parts):
    total = parts[0].astype(f32)
    for k in range(1, parts.shape[0]):
        total = total + parts[k].astype(f32)
    return total


def expand(
    parts, gains, query_up, key_gain, cosines, sines, out, rope_out, rope_tile, edges, *, width
):
    kv, batch = out.shape[0], out.shape[1]
    rows = query_up.shape[0]
    low = total_of(parts)
    lane = lane_of(batch)
    inverse = lax.rsqrt(low[:, rows : rows + 1] / width + epsilon)
    upper = low * inverse
    chosen = lax.broadcasted_iota(jnp.int32, inverse.shape, 0) == lax.axis_index("lo")
    latent = low * jnp.sum(jnp.where(chosen, inverse, 0.0), axis=0, keepdims=True)
    edges[...] = latent
    latent = shifted(latent, 1)
    query_low = jnp.where(lane < rows, upper, 0.0)
    squares = jnp.sum(query_low * query_low, axis=1, keepdims=True)
    own_gain = gains[pl.ds(lax.axis_index(KV), 1), :]
    part = dot((query_low * own_gain)[:, :rows].astype(bf16), query_up[...])
    size = NOPE + ROPE
    heads = part.shape[1] // size
    for n in range(heads):
        tile = jnp.where(
            lane < size, window(part, size * n, size), jnp.where(lane == size, squares, latent)
        ).astype(bf16)
        for k in range(n, kv, heads):
            out[k] = tile
    in_rope = (lane >= 2 * ROPE) & (lane < 3 * ROPE)
    rope = jnp.where(in_rope, upper, 0.0)
    rope = (
        rope
        * lax.rsqrt(jnp.sum(rope * rope, axis=1, keepdims=True) / ROPE + epsilon)
        * key_gain[...]
    )
    rope = shifted(rope * cosines[...] + swapped_halves(rope) * sines[...], -2 * ROPE)
    rope = jnp.where(lane < ROPE, rope, 0.0)
    rope_tile[...] = rope
    rope_out[...] = rope[:, :ROPE].astype(bf16)


def absorb(parts, key_head, gain, cosines, sines, edges, latent_gain, out, *, rank):
    total = total_of(parts)
    lane = lane_of(total.shape[0])
    size = NOPE + ROPE
    queries = total * lax.rsqrt(total[:, size : size + 1] / rank + epsilon)
    squared = queries * queries
    nope = lane < NOPE
    in_rope = (lane >= NOPE) & (lane < size)
    mean_nope = jnp.sum(jnp.where(nope, squared, 0.0), axis=1, keepdims=True) / NOPE
    mean_rope = jnp.sum(jnp.where(in_rope, squared, 0.0), axis=1, keepdims=True) / ROPE
    queries = (
        queries
        * jnp.where(nope, lax.rsqrt(mean_nope + epsilon), lax.rsqrt(mean_rope + epsilon))
        * gain[...]
    )
    rope = queries * cosines[...] + swapped_halves(queries) * sines[...]
    rope = jnp.where(lane < ROPE, shifted(rope, -NOPE), 0.0).astype(bf16)
    own = lax.dot_general(
        jnp.where(nope, queries, 0.0).astype(bf16),
        key_head[...],
        (((1,), (1,)), ((), ())),
        preferred_element_type=f32,
    ).astype(bf16)
    heads = out.shape[0]
    latent = jnp.zeros_like(total)
    for m in range(LANES // CUT):
        piece = parts[m * heads + lax.axis_index("lo")].astype(f32)
        here = (lane >= m * CUT) & (lane < m * CUT + CUT - 1)
        latent = jnp.where(here, shifted(piece, m * CUT - size - 1), latent)
        last = m * CUT + CUT - 1
        latent = jnp.where(lane == last, shifted(edges[...], last - EDGE - m), latent)
    mean = jnp.sum(jnp.sum(latent * latent, axis=1, keepdims=True), axis=0, keepdims=True) / (
        latent.shape[0] * latent.shape[1]
    )
    latent = (latent * lax.rsqrt(mean + epsilon) * latent_gain[...]).astype(bf16)
    columns = own.shape[1]
    for n in range(out.shape[0]):
        out[n, :, :columns] = own
        out[n, :, columns : columns + LANES] = rope
        out[n, :, columns + LANES :] = latent


def attend(lengths, third, cache, ropes, new_rope, out, new_latent, by_batch, all_scores, all_weights):
    heads, batch = third.shape[0], third.shape[1]
    rank = cache.shape[2]
    context = cache.shape[1]
    rows = heads * batch
    kv_index = lax.axis_index(KV)
    queries = third[...].reshape(rows, third.shape[2])
    latent_q = queries[:, :rank]
    rope_q = queries[:, rank : rank + LANES]
    by_batch[...] = third[:, :, rank + LANES :].astype(f32)
    fresh_latent = jnp.concatenate([by_batch[:, j, :] for j in range(batch)], axis=1)
    new_latent[...] = fresh_latent.astype(bf16)
    tiled = jnp.concatenate([fresh_latent] * heads, axis=0)
    tiled_rope = jnp.concatenate([new_rope[...].astype(bf16).astype(f32)] * heads, axis=0)
    scale = (NOPE + ROPE) ** (-0.5)
    fresh = (
        jnp.sum(latent_q.astype(f32) * tiled, axis=1, keepdims=True)
        + jnp.sum(rope_q.astype(f32) * tiled_rope, axis=1, keepdims=True)
    ) * scale
    leader = kv_index == 0
    fresh = jnp.where(leader, fresh, lowest)
    of_row = lax.broadcasted_iota(jnp.int32, (rows, 1), 0) % batch
    limit = jnp.zeros((rows, 1), jnp.int32)
    for b in range(batch):
        limit = jnp.where(of_row == b, lengths[b], limit)

    @pl.when(kv_index >= 0)
    def _():
        scores = jnp.zeros((rows, context), f32)
        for b in range(batch):
            part = lax.dot_general(
                latent_q, cache[b], (((1,), (1,)), ((), ())), preferred_element_type=f32
            ) + dot(rope_q[:, :ROPE], ropes[b])
            scores = jnp.where(of_row == b, part, scores)
        all_scores[...] = scores

    scores = all_scores[...]
    positions = kv_index * context + lax.broadcasted_iota(jnp.int32, (rows, context), 1)
    usable = positions < limit
    masked = jnp.where(usable, scores * scale, lowest)
    top = jnp.maximum(jnp.max(masked, axis=1, keepdims=True), fresh)
    top_hi, top_lo = split_two(top)
    top = top_hi + top_lo
    weights = jnp.where(usable, jnp.exp(masked - top), 0.0)
    fresh_weight = jnp.where(leader, jnp.exp(fresh - top), 0.0)
    totals = jnp.sum(weights, axis=1, keepdims=True) + fresh_weight
    all_weights[...] = weights
    total_hi, total_lo = split_two(totals)
    lane = lane_of(rows)
    stats = jnp.where(
        lane == 0,
        top_hi,
        jnp.where(lane == 1, top_lo, jnp.where(lane == 2, total_hi, total_lo)),
    )

    @pl.when(kv_index >= 0)
    def _():
        summed = fresh_weight.astype(bf16).astype(f32) * tiled
        for b in range(batch):
            own = jnp.where(of_row == b, all_weights[...], 0.0).astype(bf16)
            summed = summed + dot(own, cache[b])
        out[:, :, :rank] = summed.astype(bf16).reshape(heads, batch, rank)

    out[:, :, rank:] = stats.astype(bf16).reshape(heads, batch, LANES)


def combine(fourth, value_head, out):
    sources, batch = fourth.shape[0], fourth.shape[1]
    rank = value_head.shape[0]
    stats = fourth[:, :, rank:].astype(f32)
    tops = stats[:, :, 0:1] + stats[:, :, 1:2]
    part_totals = stats[:, :, 2:3] + stats[:, :, 3:4]
    top_hi, top_lo = split_two(jnp.max(tops, axis=0))
    factors = jnp.exp(tops - (top_hi + top_lo)[None])
    totals = jnp.sum(part_totals * factors, axis=0)
    summed = factors[0] * fourth[0, :, :rank].astype(f32)
    for s in range(1, sources):
        summed = summed + factors[s] * fourth[s, :, :rank].astype(f32)
    latent_out = (summed / jnp.where(totals > 0.0, totals, 1.0)).astype(bf16)
    head = dot(latent_out, value_head[...])
    total_hi, total_lo = split_two(totals)
    lane = lane_of(batch)
    tile = jnp.where(
        lane < VDIM,
        head,
        jnp.where(
            lane == VDIM,
            top_hi,
            jnp.where(lane == VDIM + 1, top_lo, jnp.where(lane == VDIM + 2, total_hi, total_lo)),
        ),
    ).astype(bf16)
    for k in range(out.shape[0]):
        out[k] = tile


def project(fifth, output_proj, out):
    kv, batch = fifth.shape[0], fifth.shape[1]
    heads = output_proj.shape[0] // VDIM
    blocks = fifth[...].astype(f32).reshape(kv // heads, heads, batch, LANES)
    tops = blocks[..., VDIM : VDIM + 1] + blocks[..., VDIM + 1 : VDIM + 2]
    factors = jnp.exp(tops - jnp.max(tops, axis=0, keepdims=True)) * (
        blocks[..., VDIM + 2 : VDIM + 3] + blocks[..., VDIM + 3 : VDIM + 4]
    )
    heads_out = jnp.sum(blocks * factors, axis=0) / jnp.sum(factors, axis=0)
    low_lane = lane_of(batch) < VDIM
    tiles = [
        jnp.where(low_lane, heads_out[n], shifted(heads_out[n + 1], VDIM))
        for n in range(0, heads, 2)
    ]
    result = dot(jnp.concatenate(tiles, axis=1).astype(bf16), output_proj[...]).astype(bf16)
    for t in range(out.shape[0]):
        out[t] = result


def finish(parts, out):
    total = total_of(parts)
    columns = out.shape[1]
    index = lax.axis_index("tp")
    result = total[:, :columns]
    for t in range(1, LANES // columns):
        result = jnp.where(index == t, shifted(total, -t * columns)[:, :columns], result)
    out[...] = result.astype(bf16)


def body(
    tokens,
    input_gain,
    query_down,
    latent_down,
    query_gain,
    query_up,
    nope_gain,
    query_rope_gain,
    key_up,
    latent_gain,
    key_rope_gain,
    latent_cache,
    rope_cache,
    lengths,
    value_up,
    output_proj,
):
    batch = tokens.shape[0]
    kv = lax.axis_size(KV)
    lo = lax.axis_size("lo")
    tp = lax.axis_size("tp")
    width = tokens.shape[1] * kv * tp
    heads = query_up.shape[1] // (NOPE + ROPE)
    own_rows = query_up.shape[0]
    q_rank = own_rows * kv
    kv_rank = latent_cache.shape[2]
    half = key_up.shape[0] // 2
    assert heads == lo == batch == 8 and kv_rank == 8 * LANES and tp == 4

    def shape(*dims, dtype=bf16):
        return jax.ShapeDtypeStruct(dims, dtype)

    lanes = jnp.arange(LANES)
    angles = lengths.astype(f32)[:, None] * theta ** (
        -(lanes % (ROPE // 2)).astype(f32) / (ROPE // 2)
    )
    cosines = jnp.cos(angles)
    sines = jnp.sin(angles) * jnp.where(lanes % ROPE < ROPE // 2, -1.0, 1.0)
    gains = jnp.pad(query_gain.reshape(kv, own_rows), ((0, 0), (0, LANES - own_rows)))
    head_gain = jnp.pad(jnp.concatenate([nope_gain, query_rope_gain]), (0, ROPE))[None]
    key_gain = jnp.pad(key_rope_gain, (2 * ROPE, ROPE))[None]

    first = exchange(
        run(
            compress,
            shape(kv, batch + 2 * half, LANES),
            tokens,
            input_gain[None],
            query_down,
            latent_down,
            key_up,
            value_up,
            scratch=[pltpu.VMEM((batch, 8, LANES), f32)],
            vmem=60 << 20,
        ),
        KV,
    )
    low, key_head, value_head = run(
        gathered,
        (shape(tp, batch, LANES), shape(kv_rank, LANES), shape(kv_rank, LANES)),
        first,
        cosines,
        sines,
        gains,
        head_gain,
        key_gain,
        flops=FLOPS,
    )
    low = exchange(low, "tp")

    second, new_rope_key, rope_tile, edges = run(
        lambda *refs: expand(*refs, width=width),
        (
            shape(kv, batch, LANES),
            shape(batch, ROPE),
            shape(batch, LANES, dtype=f32),
            shape(batch, LANES, dtype=f32),
        ),
        low,
        gains,
        query_up,
        key_gain,
        cosines,
        sines,
        flops=FLOPS,
    )
    second = exchange(second, KV)
    third = exchange(
        run(
            lambda *refs: absorb(*refs, rank=q_rank),
            shape(lo, batch, kv_rank + 2 * LANES),
            second,
            key_head,
            head_gain,
            cosines,
            sines,
            edges,
            latent_gain.reshape(8, LANES),
            flops=FLOPS,
        ),
        "lo",
    )
    fourth, new_latent = run(
        attend,
        (shape(heads, batch, kv_rank + LANES), shape(batch, kv_rank)),
        lengths,
        third,
        latent_cache,
        rope_cache,
        rope_tile,
        scratch=[
            pltpu.VMEM((batch, 8, LANES), f32),
            pltpu.VMEM((heads * batch, latent_cache.shape[1]), f32),
            pltpu.VMEM((heads * batch, latent_cache.shape[1]), f32),
        ],
        smem=(0,),
    )
    fourth = exchange(fourth, "lo")
    fifth = exchange(run(combine, shape(kv, batch, LANES), fourth, value_head), KV)
    partial = run(project, shape(tp, batch, output_proj.shape[1]), fifth, output_proj)
    attended = run(finish, shape(batch, output_proj.shape[1] // tp), exchange(partial, "tp"))
    return (attended, new_latent, new_rope_key)


def solution(mesh):
    kv, lo = mesh.shape["kv"], 8
    split = Mesh(
        mesh.devices.reshape(mesh.shape["grp"], kv // lo, lo, mesh.shape["tp"]),
        ("grp", "hi", "lo", "tp"),
    )
    placed = (
        P("grp", KV_TP),
        P(KV_TP),
        P(KV_TP, None),
        P(KV_TP, None),
        P(),
        P(KV, "tp"),
        P(),
        P(),
        P(KV, "tp"),
        P(),
        P(),
        P("grp", KV, None),
        P("grp", None, KV),
        P("grp"),
        P(KV, "tp"),
        P("tp", KV),
    )
    return jax.shard_map(
        body,
        mesh=split,
        in_specs=placed,
        out_specs=(P("grp", KV_TP), P("grp", None), P("grp", None)),
        check_vma=False,
    )
```

```python
import jax
import jax.numpy as jnp
from jax import lax
from jax.experimental import pallas as pl
from jax.experimental.pallas import tpu as pltpu
from jax.sharding import Mesh
from jax.sharding import PartitionSpec as P

NOPE = 64
ROPE = 32
VDIM = 64
LANES = 128
CUT = 32
EDGE = 52
KV = ("hi", "lo")
KV_TP = ("hi", "lo", "tp")

epsilon = 1e-06
theta = 10000.0
lowest = -1e30

f32 = jnp.float32
bf16 = jnp.bfloat16

FLOPS = 1 << 32
VMEM_LIMIT = 16 << 20
IN_VMEM = pl.BlockSpec(memory_space=pltpu.VMEM)
IN_SMEM = pl.BlockSpec(memory_space=pltpu.SMEM)


def run(kernel, outs, *args, scratch=(), smem=(), vmem=VMEM_LIMIT, flops=0):
    return pl.pallas_call(
        kernel,
        out_shape=outs,
        in_specs=[IN_SMEM if i in smem else IN_VMEM for i in range(len(args))],
        out_specs=jax.tree.map(lambda _: IN_VMEM, outs),
        scratch_shapes=scratch,
        compiler_params=pltpu.CompilerParams(vmem_limit_bytes=vmem),
        cost_estimate=pl.CostEstimate(flops=flops, transcendentals=0, bytes_accessed=0),
    )(*args)


def exchange(x, axes):
    return lax.all_to_all(x, axes, 0, 0, tiled=True)


def lane_of(rows):
    return lax.broadcasted_iota(jnp.int32, (rows, LANES), 1)


def shifted(x, amount):
    return pltpu.roll(x, amount % LANES, 1) if amount % LANES else x


def window(x, start, length):
    tile, off = divmod(start, LANES)
    first = shifted(x[:, tile * LANES : (tile + 1) * LANES], -off)
    if off + length <= LANES:
        return first
    second = shifted(x[:, (tile + 1) * LANES : (tile + 2) * LANES], -off)
    return jnp.where(lane_of(x.shape[0]) < LANES - off, first, second)


def swapped_halves(x):
    half = ROPE // 2
    return jnp.where(lane_of(x.shape[0]) % ROPE < half, shifted(x, -half), shifted(x, half))


def split_two(x):
    top = x.astype(bf16).astype(f32)
    return top, (x - top).astype(bf16).astype(f32)


def dot(a, b):
    return jnp.dot(a, b, preferred_element_type=f32)


def compress(tokens, gain, query_down, latent_down, key_up, value_up, out, by_batch):
    kv, batch = out.shape[0], tokens.shape[0]
    heads = by_batch.shape[0]
    own = query_down.shape[1] // kv
    values = tokens[...].astype(f32)
    scaled = (values * gain[...]).astype(bf16)
    squares = jnp.sum(values * values, axis=1, keepdims=True)
    part_q = dot(scaled, query_down[...])
    part_l = dot(scaled, latent_down[...])
    lane = lane_of(batch)
    rest = jnp.concatenate([part_l[:, 8 * LANES :], jnp.zeros((batch, LANES - ROPE), f32)], axis=1)
    fixed = jnp.where(lane < 2 * ROPE, squares, shifted(rest, 2 * ROPE))
    for j in range(8):
        by_batch[:, j, :] = part_l[:, j * LANES : (j + 1) * LANES]
    for n in range(heads):
        latent = by_batch[n]
        shared = fixed
        for m in range(LANES // CUT):
            shared = jnp.where(
                lane == EDGE + m, shifted(latent, EDGE + m - (m * CUT + CUT - 1)), shared
            )
        for k in range(n, kv, heads):
            tile = jnp.where(lane < own, window(part_q, own * k, own), shared)
            tile = jnp.where(
                lane < LANES - CUT, tile, shifted(latent, LANES - CUT - k // heads * CUT)
            )
            out[k, 0:8, :] = tile.astype(bf16)
    half = key_up.shape[0] // 2
    low_lane = lane_of(half) < NOPE
    for row, weights in ((8, key_up), (8 + half, value_up)):
        for j in range(heads // 2):
            upper = weights[0:half, j * LANES : (j + 1) * LANES].astype(f32)
            lower = weights[half:, j * LANES : (j + 1) * LANES].astype(f32)
            pair = (
                jnp.where(low_lane, upper, shifted(lower, NOPE)).astype(bf16),
                jnp.where(low_lane, shifted(upper, NOPE), lower).astype(bf16),
            )
            for n in (0, 1):
                for k in range(2 * j + n, kv, heads):
                    out[k, row : row + half, :] = pair[n]


def gathered(first, *refs):
    low, key_head, value_head = refs[-3:]
    half = key_head.shape[0] // first.shape[0] // 2
    total = first[0, 0:8, :].astype(f32)
    for k in range(1, first.shape[0]):
        total = total + first[k, 0:8, :].astype(f32)
    for t in range(low.shape[0]):
        low[t] = total.astype(bf16)
    for k in range(first.shape[0]):
        for row, out in ((8, key_head), (8 + half, value_head)):
            tile = first[k, row : row + half, :]
            out[2 * half * k : 2 * half * k + half, :] = tile
            out[2 * half * k + half : 2 * half * (k + 1), :] = shifted(
                tile.astype(f32), NOPE
            ).astype(bf16)


def total_of(parts):
    total = parts[0].astype(f32)
    for k in range(1, parts.shape[0]):
        total = total + parts[k].astype(f32)
    return total


def expand(
    parts, gains, query_up, key_gain, cosines, sines, out, rope_tile, edges, *, width
):
    kv, batch = out.shape[0], out.shape[1]
    rows = query_up.shape[0]
    low = total_of(parts)
    lane = lane_of(batch)
    inverse = lax.rsqrt(low[:, rows : rows + 1] / width + epsilon)
    upper = low * inverse
    chosen = lax.broadcasted_iota(jnp.int32, inverse.shape, 0) == lax.axis_index("lo")
    latent = low * jnp.sum(jnp.where(chosen, inverse, 0.0), axis=0, keepdims=True)
    edges[...] = latent
    latent = shifted(latent, 1)
    query_low = jnp.where(lane < rows, upper, 0.0)
    squares = jnp.sum(query_low * query_low, axis=1, keepdims=True)
    own_gain = gains[pl.ds(lax.axis_index(KV), 1), :]
    part = dot((query_low * own_gain)[:, :rows].astype(bf16), query_up[...])
    size = NOPE + ROPE
    heads = part.shape[1] // size
    for n in range(heads):
        tile = jnp.where(
            lane < size, window(part, size * n, size), jnp.where(lane == size, squares, latent)
        ).astype(bf16)
        for k in range(n, kv, heads):
            out[k] = tile
    in_rope = (lane >= 2 * ROPE) & (lane < 3 * ROPE)
    rope = jnp.where(in_rope, upper, 0.0)
    rope = (
        rope
        * lax.rsqrt(jnp.sum(rope * rope, axis=1, keepdims=True) / ROPE + epsilon)
        * key_gain[...]
    )
    rope = shifted(rope * cosines[...] + swapped_halves(rope) * sines[...], -2 * ROPE)
    rope = jnp.where(lane < ROPE, rope, 0.0)
    rope_tile[...] = rope.astype(bf16).astype(f32)


def absorb(parts, key_head, gain, cosines, sines, edges, latent_gain, out, *, rank):
    total = total_of(parts)
    lane = lane_of(total.shape[0])
    size = NOPE + ROPE
    queries = total * lax.rsqrt(total[:, size : size + 1] / rank + epsilon)
    squared = queries * queries
    nope = lane < NOPE
    in_rope = (lane >= NOPE) & (lane < size)
    mean_nope = jnp.sum(jnp.where(nope, squared, 0.0), axis=1, keepdims=True) / NOPE
    mean_rope = jnp.sum(jnp.where(in_rope, squared, 0.0), axis=1, keepdims=True) / ROPE
    queries = (
        queries
        * jnp.where(nope, lax.rsqrt(mean_nope + epsilon), lax.rsqrt(mean_rope + epsilon))
        * gain[...]
    )
    rope = queries * cosines[...] + swapped_halves(queries) * sines[...]
    rope = jnp.where(lane < ROPE, shifted(rope, -NOPE), 0.0).astype(bf16)
    own = lax.dot_general(
        jnp.where(nope, queries, 0.0).astype(bf16),
        key_head[...],
        (((1,), (1,)), ((), ())),
        preferred_element_type=f32,
    ).astype(bf16)
    heads = out.shape[0]
    latent = jnp.zeros_like(total)
    for m in range(LANES // CUT):
        piece = parts[m * heads + lax.axis_index("lo")].astype(f32)
        here = (lane >= m * CUT) & (lane < m * CUT + CUT - 1)
        latent = jnp.where(here, shifted(piece, m * CUT - size - 1), latent)
        last = m * CUT + CUT - 1
        latent = jnp.where(lane == last, shifted(edges[...], last - EDGE - m), latent)
    mean = jnp.sum(jnp.sum(latent * latent, axis=1, keepdims=True), axis=0, keepdims=True) / (
        latent.shape[0] * latent.shape[1]
    )
    latent = (latent * lax.rsqrt(mean + epsilon) * latent_gain[...]).astype(bf16)
    columns = own.shape[1]
    for n in range(out.shape[0]):
        out[n, :, :columns] = own
        out[n, :, columns : columns + LANES] = rope
        out[n, :, columns + LANES :] = latent


def soften(
    lengths, third, products, ropes, new_rope, weights_out, fresh_out, stats_out, new_latent, wide, tail
):
    heads, batch = third.shape[0], third.shape[1]
    rank = new_latent.shape[1]
    context = products.shape[2]
    kv_index = lax.axis_index(KV)
    leader = kv_index == 0
    scale = (NOPE + ROPE) ** (-0.5)
    wide[...] = third[:, :, : rank + LANES].astype(f32)
    tail[...] = third[:, :, rank + LANES :].astype(f32)
    latent = jnp.concatenate([tail[:, j, :] for j in range(rank // LANES)], axis=1)
    new_latent[...] = latent.astype(bf16)
    positions = kv_index * context + lax.broadcasted_iota(jnp.int32, (heads, context), 1)
    lane = lane_of(heads)
    for b in range(batch):
        query = wide[:, b, :]
        rope = query[:, rank:]
        scores = products[b] + dot(rope[:, :ROPE].astype(bf16), ropes[b])
        fresh = (
            jnp.sum(query[:, :rank] * latent[b : b + 1], axis=1, keepdims=True)
            + jnp.sum(rope * new_rope[b : b + 1, :], axis=1, keepdims=True)
        ) * scale
        fresh = jnp.where(leader, fresh, lowest)
        usable = positions < lengths[b]
        masked = jnp.where(usable, scores * scale, lowest)
        top_hi, top_lo = split_two(
            jnp.maximum(jnp.max(masked, axis=1, keepdims=True), fresh)
        )
        top = top_hi + top_lo
        weights = jnp.where(usable, jnp.exp(masked - top), 0.0)
        fresh_weight = jnp.where(leader, jnp.exp(fresh - top), 0.0)
        total_hi, total_lo = split_two(jnp.sum(weights, axis=1, keepdims=True) + fresh_weight)
        weights_out[b] = weights.astype(bf16)
        fresh_out[b] = jnp.broadcast_to(fresh_weight.astype(bf16).astype(f32), (heads, LANES))
        stats_out[:, b, :] = jnp.where(
            lane == 0,
            top_hi,
            jnp.where(lane == 1, top_lo, jnp.where(lane == 2, total_hi, total_lo)),
        )


def assemble(summed, fresh, stats, new_latent, out, wide):
    batch, heads, rank = summed.shape
    for b in range(batch):
        latent = new_latent[...].astype(f32)[b : b + 1]
        wide[:, b, :] = summed[b] + fresh[b][:, 0:1] * latent
    out[:, :, :rank] = wide[...].astype(bf16)
    out[:, :, rank:] = stats[...].astype(bf16)


def combine(fourth, value_head, out):
    sources, batch = fourth.shape[0], fourth.shape[1]
    rank = value_head.shape[0]
    stats = fourth[:, :, rank:].astype(f32)
    tops = stats[:, :, 0:1] + stats[:, :, 1:2]
    part_totals = stats[:, :, 2:3] + stats[:, :, 3:4]
    top_hi, top_lo = split_two(jnp.max(tops, axis=0))
    factors = jnp.exp(tops - (top_hi + top_lo)[None])
    totals = jnp.sum(part_totals * factors, axis=0)
    summed = factors[0] * fourth[0, :, :rank].astype(f32)
    for s in range(1, sources):
        summed = summed + factors[s] * fourth[s, :, :rank].astype(f32)
    latent_out = (summed / jnp.where(totals > 0.0, totals, 1.0)).astype(bf16)
    head = dot(latent_out, value_head[...])
    total_hi, total_lo = split_two(totals)
    lane = lane_of(batch)
    tile = jnp.where(
        lane < VDIM,
        head,
        jnp.where(
            lane == VDIM,
            top_hi,
            jnp.where(lane == VDIM + 1, top_lo, jnp.where(lane == VDIM + 2, total_hi, total_lo)),
        ),
    ).astype(bf16)
    for k in range(out.shape[0]):
        out[k] = tile


def project(fifth, output_proj, out):
    kv, batch = fifth.shape[0], fifth.shape[1]
    heads = output_proj.shape[0] // VDIM
    blocks = fifth[...].astype(f32).reshape(kv // heads, heads, batch, LANES)
    tops = blocks[..., VDIM : VDIM + 1] + blocks[..., VDIM + 1 : VDIM + 2]
    factors = jnp.exp(tops - jnp.max(tops, axis=0, keepdims=True)) * (
        blocks[..., VDIM + 2 : VDIM + 3] + blocks[..., VDIM + 3 : VDIM + 4]
    )
    heads_out = jnp.sum(blocks * factors, axis=0) / jnp.sum(factors, axis=0)
    low_lane = lane_of(batch) < VDIM
    tiles = [
        jnp.where(low_lane, heads_out[n], shifted(heads_out[n + 1], VDIM))
        for n in range(0, heads, 2)
    ]
    result = dot(jnp.concatenate(tiles, axis=1).astype(bf16), output_proj[...]).astype(bf16)
    for t in range(out.shape[0]):
        out[t] = result


def finish(parts, latent, rope, out, latent_out, rope_out):
    latent_out[...] = latent[...]
    rope_out[...] = rope[:, : rope_out.shape[1]].astype(bf16)
    total = total_of(parts)
    columns = out.shape[1]
    index = lax.axis_index("tp")
    result = total[:, :columns]
    for t in range(1, LANES // columns):
        result = jnp.where(index == t, shifted(total, -t * columns)[:, :columns], result)
    out[...] = result.astype(bf16)


def body(
    tokens,
    input_gain,
    query_down,
    latent_down,
    query_gain,
    query_up,
    nope_gain,
    query_rope_gain,
    key_up,
    latent_gain,
    key_rope_gain,
    latent_cache,
    rope_cache,
    lengths,
    value_up,
    output_proj,
):
    batch = tokens.shape[0]
    kv = lax.axis_size(KV)
    lo = lax.axis_size("lo")
    tp = lax.axis_size("tp")
    width = tokens.shape[1] * kv * tp
    heads = query_up.shape[1] // (NOPE + ROPE)
    own_rows = query_up.shape[0]
    q_rank = own_rows * kv
    kv_rank = latent_cache.shape[2]
    half = key_up.shape[0] // 2
    assert heads == lo == batch == 8 and kv_rank == 8 * LANES and tp == 4

    def shape(*dims, dtype=bf16):
        return jax.ShapeDtypeStruct(dims, dtype)

    lanes = jnp.arange(LANES)
    angles = lengths.astype(f32)[:, None] * theta ** (
        -(lanes % (ROPE // 2)).astype(f32) / (ROPE // 2)
    )
    cosines = jnp.cos(angles)
    sines = jnp.sin(angles) * jnp.where(lanes % ROPE < ROPE // 2, -1.0, 1.0)
    gains = jnp.pad(query_gain.reshape(kv, own_rows), ((0, 0), (0, LANES - own_rows)))
    head_gain = jnp.pad(jnp.concatenate([nope_gain, query_rope_gain]), (0, ROPE))[None]
    key_gain = jnp.pad(key_rope_gain, (2 * ROPE, ROPE))[None]

    first = exchange(
        run(
            compress,
            shape(kv, batch + 2 * half, LANES),
            tokens,
            input_gain[None],
            query_down,
            latent_down,
            key_up,
            value_up,
            scratch=[pltpu.VMEM((batch, 8, LANES), f32)],
            vmem=60 << 20,
        ),
        KV,
    )
    low, key_head, value_head = run(
        gathered,
        (shape(tp, batch, LANES), shape(kv_rank, LANES), shape(kv_rank, LANES)),
        first,
        cosines,
        sines,
        gains,
        head_gain,
        key_gain,
        flops=FLOPS,
    )
    low = exchange(low, "tp")

    second, rope_tile, edges = run(
        lambda *refs: expand(*refs, width=width),
        (
            shape(kv, batch, LANES),
            shape(batch, LANES, dtype=f32),
            shape(batch, LANES, dtype=f32),
        ),
        low,
        gains,
        query_up,
        key_gain,
        cosines,
        sines,
        flops=FLOPS,
    )
    second = exchange(second, KV)
    third = exchange(
        run(
            lambda *refs: absorb(*refs, rank=q_rank),
            shape(lo, batch, kv_rank + 2 * LANES),
            second,
            key_head,
            head_gain,
            cosines,
            sines,
            edges,
            latent_gain.reshape(8, LANES),
            flops=FLOPS,
        ),
        "lo",
    )
    products = jnp.einsum(
        "hbr,bpr->bhp", third[:, :, :kv_rank], latent_cache, preferred_element_type=f32
    )
    context = latent_cache.shape[1]
    weights, fresh, stats, new_latent = run(
        soften,
        (
            shape(batch, heads, context),
            shape(batch, heads, LANES, dtype=f32),
            shape(heads, batch, LANES, dtype=f32),
            shape(batch, kv_rank),
        ),
        lengths,
        third,
        products,
        rope_cache,
        rope_tile,
        scratch=[
            pltpu.VMEM((heads, batch, kv_rank + LANES), f32),
            pltpu.VMEM((batch, 8, LANES), f32),
        ],
        smem=(0,),
    )
    summed = jnp.einsum("bhp,bpr->bhr", weights, latent_cache, preferred_element_type=f32)
    fourth = run(
        assemble,
        shape(heads, batch, kv_rank + LANES),
        summed,
        fresh,
        stats,
        new_latent,
        scratch=[pltpu.VMEM((heads, batch, kv_rank), f32)],
    )
    fourth = exchange(fourth, "lo")
    fifth = exchange(run(combine, shape(kv, batch, LANES), fourth, value_head), KV)
    partial = run(project, shape(tp, batch, output_proj.shape[1]), fifth, output_proj)
    return run(
        finish,
        (shape(batch, output_proj.shape[1] // tp), shape(batch, kv_rank), shape(batch, ROPE)),
        exchange(partial, "tp"),
        new_latent,
        rope_tile,
    )


def solution(mesh):
    kv, lo = mesh.shape["kv"], 8
    split = Mesh(
        mesh.devices.reshape(mesh.shape["grp"], kv // lo, lo, mesh.shape["tp"]),
        ("grp", "hi", "lo", "tp"),
    )
    placed = (
        P("grp", KV_TP),
        P(KV_TP),
        P(KV_TP, None),
        P(KV_TP, None),
        P(),
        P(KV, "tp"),
        P(),
        P(),
        P(KV, "tp"),
        P(),
        P(),
        P("grp", KV, None),
        P("grp", None, KV),
        P("grp"),
        P(KV, "tp"),
        P("tp", KV),
    )
    return jax.shard_map(
        body,
        mesh=split,
        in_specs=placed,
        out_specs=(P("grp", KV_TP), P("grp", None), P("grp", None)),
        check_vma=False,
    )
```
